32 devices in a mesh: grp: 2 (over y), ep: 8 (over z, x), tp: 2 (over core).
Axes of the slice: x: 2, y: 2, z: 4, core: 2. Of those that a mesh axis runs over, the one named last changes fastest.
Arguments:
- tokens: bfloat16 [1024, 2048], P(('grp', 'ep')), parts along dimension 0, may hold values from -6 to 6
- chosen: int32 [1, 16, 9], P(None, ('grp', 'ep')), parts along dimension 1, may hold values from -1 to 63, as said below
- route_weight: float32 [1, 16, 9], P(None, ('grp', 'ep')), parts along dimension 1, may hold values from 0.1 to 1
- expert_gate: bfloat16 [2048, 4096], P(None, ('ep', 'tp')), may hold values from -0.125 to 0.125
- expert_up: bfloat16 [2048, 4096], P(None, ('ep', 'tp')), may hold values from -0.125 to 0.125
- expert_down: bfloat16 [4096, 2048], P(('ep', 'tp')), may hold values from -0.09375 to 0.09375
- dense_gate: bfloat16 [2048, 512], P('ep', 'tp'), may hold values from -0.125 to 0.125
- dense_up: bfloat16 [2048, 512], P('ep', 'tp'), may hold values from -0.125 to 0.125
- dense_down: bfloat16 [512, 2048], P('tp', 'ep'), may hold values from -0.25 to 0.25
- branch_gate: float32 [2048], P('tp'), may hold values from -6 to 6
Outputs:
- mixed: bfloat16 [1024, 2048], P(('grp', 'ep'), 'tp'), parts along dimension 0
The draws below stay inside these ranges and needn't reach their ends.
There are 2 independent parts, one for each index of `grp`. The reference program is written for one: setup_inputs(seed, part) draws one part's arguments, and reference() takes and returns one part's arrays. A program takes and returns all parts, laid end to end along the dimension named above; an argument that names none is the same for every part. Nothing has to cross between parts.
Inputs may be any that keep to these rules, and one draw needn't show every extreme that they name: chosen[e, s, k] is -1 or an index local to device s (token s * 64 + chosen[e, s, k] of the whole). In each (e, s) row the live entries come first and are distinct, the -1 entries follow. Each expert takes exactly 64 tokens in all, at most 9 from one device, and for every expert some device gives it exactly 9.
All inputs are finite; a program needn't handle non-finite values.
Results may differ from the reference program's by a relative error of at most 0.0085.
Values may be sent and summed in bfloat16 or wider, within the bound.
No kernel may reach another device: no remote copies, remote signals or barrier semaphores. Data moves between devices by JAX's collectives and lax.ppermute only.
A program may use at most 64 MiB of HBM per device.

```python
import jax
import jax.numpy as jnp
from jax import lax

D = 2048
FF = 4096
DH = 512
TOK_DEV = 64
EXPERTS = 1
SLOT = 9
TOKENS = 512
N_EP = 8


def draw_chosen(key, part):
    middle = TOK_DEV // 8
    spread = SLOT - middle
    pairs = N_EP // 2
    base = jax.random.fold_in(key, 17)
    key_shift = jax.random.fold_in(base, 1)
    key_top = jax.random.fold_in(base, 2)
    key_order = jax.random.fold_in(base, 3)
    shift = jax.random.randint(key_shift, (EXPERTS, pairs), -spread, spread + 1)
    top_pair = jax.random.randint(key_top, (EXPERTS,), 0, pairs)
    shift = jnp.where(jnp.arange(pairs)[None, :] == top_pair[:, None], spread, shift)
    counts = jnp.stack([middle + shift, middle - shift], axis=-1).reshape(EXPERTS, N_EP)
    order_keys = jax.random.split(key_order, EXPERTS * N_EP)
    orders = jax.vmap(lambda single: jax.random.permutation(single, TOK_DEV))(order_keys).reshape(EXPERTS, N_EP, TOK_DEV)
    slots_iota = jnp.arange(SLOT)
    return jnp.where(slots_iota[None, None, :] < counts[:, :, None], orders[:, :, :SLOT], -1).astype(jnp.int32)


def levels(rng, dims, cuts, least, largest):
    factor_of, own = 1.0, jax.random.fold_in(rng, 6)
    for axis_at, blocks in cuts:
        steps = jnp.exp(jax.random.uniform(jax.random.fold_in(own, axis_at), (blocks,), jnp.float32, least / len(cuts), largest / len(cuts)))
        factor_of = factor_of * jnp.repeat(steps, dims[axis_at] // blocks).reshape([-1 if axis == axis_at else 1 for axis in range(len(dims))])
    return factor_of


def normal_values(key, dims, scale, bound, shards=(), held_as=jnp.bfloat16):
    result = scale * jax.random.normal(key, dims, jnp.float32)
    if shards:
        result = result * levels(key, dims, shards, -0.22, 0.18)
    return jnp.clip(result, -bound, bound).astype(held_as)


def setup_inputs(seed: int = 0, part: int = 0) -> dict:
    key_of = jax.random.split(jax.random.key(seed), 11)
    part_keys = jax.random.split(jax.random.fold_in(key_of[10], part), 11)
    return {
        "tokens": normal_values(part_keys[0], (TOKENS, D), 1.0, 6.0, ((0, 8),)),
        "chosen": draw_chosen(jax.random.fold_in(jax.random.fold_in(key_of[10], part), 71), part),
        "route_weight": jnp.clip(0.1 + 0.9 * jax.random.uniform(part_keys[2], (EXPERTS, N_EP, SLOT), jnp.float32) ** levels(part_keys[2], (EXPERTS, N_EP, SLOT), ((1, 8),), -0.2, 0.2), 0.1, 1.0),
        "expert_gate": normal_values(key_of[3], (D, EXPERTS * FF), D ** -0.5, 0.125, ((1, 16),)),
        "expert_up": normal_values(key_of[4], (D, EXPERTS * FF), D ** -0.5, 0.125, ((1, 16),)),
        "expert_down": normal_values(key_of[5], (EXPERTS * FF, D), FF ** -0.5, 0.09375, ((0, 16),)),
        "dense_gate": normal_values(key_of[6], (D, DH), D ** -0.5, 0.125, ((0, 8), (1, 2))),
        "dense_up": normal_values(key_of[7], (D, DH), D ** -0.5, 0.125, ((0, 8), (1, 2))),
        "dense_down": normal_values(key_of[8], (DH, D), DH ** -0.5, 0.25, ((0, 2), (1, 8))),
        "branch_gate": normal_values(key_of[9], (D,), 2.0, 6.0, ((0, 2),), jnp.float32),
    }


def reference(tokens, chosen, route_weight, expert_gate, expert_up, expert_down, dense_gate, dense_up, dense_down, branch_gate):
    rows_all = N_EP * SLOT
    offsets = (jnp.arange(N_EP, dtype=jnp.int32) * TOK_DEV)[:, None]

    def one_expert(totals, expert_id):
        picked = lax.dynamic_index_in_dim(chosen, expert_id, 0, keepdims=False)
        filled = picked >= 0
        token_index = (jnp.maximum(picked, 0) + offsets).reshape(-1).astype(jnp.int32)
        token_rows = jnp.where(filled.reshape(-1)[:, None], tokens[token_index], jnp.zeros((), jnp.bfloat16))
        first = (expert_id * FF).astype(jnp.int32)
        gate_cols = lax.dynamic_slice_in_dim(expert_gate, first, FF, 1)
        up_cols = lax.dynamic_slice_in_dim(expert_up, first, FF, 1)
        gate_act = jnp.dot(token_rows, gate_cols, preferred_element_type=jnp.float32)
        up_act = jnp.dot(token_rows, up_cols, preferred_element_type=jnp.float32)
        hidden = (jax.nn.silu(gate_act) * up_act).astype(jnp.bfloat16)
        down_rows = lax.dynamic_slice_in_dim(expert_down, first, FF, 0).reshape(16, FF // 16, D)
        block_sums = jnp.einsum("rbh,bhd->brd", hidden.reshape(rows_all, 16, FF // 16).astype(jnp.float32), down_rows.astype(jnp.float32)).astype(jnp.bfloat16)
        block_sums = lax.optimization_barrier(block_sums)
        members = block_sums.astype(jnp.float32).reshape(8, 2, rows_all, D).sum(axis=1).astype(jnp.bfloat16)
        members = lax.optimization_barrier(members)
        expert_out = members.astype(jnp.float32).sum(axis=0)
        scale = (lax.dynamic_index_in_dim(route_weight, expert_id, 0, keepdims=False) * filled).reshape(-1)
        totals = totals.at[token_index].add(expert_out * scale[:, None])
        return totals, None

    combined, _ = lax.scan(one_expert, jnp.zeros((N_EP * TOK_DEV, D), jnp.float32), jnp.arange(EXPERTS, dtype=jnp.int32))
    gate_dense = jnp.dot(tokens, dense_gate, preferred_element_type=jnp.float32)
    up_dense = jnp.dot(tokens, dense_up, preferred_element_type=jnp.float32)
    dense_hidden = (jax.nn.silu(gate_dense) * up_dense).astype(jnp.bfloat16)
    half = DH // 2
    first_part = jnp.dot(dense_hidden[:, :half], dense_down[:half], preferred_element_type=jnp.float32).astype(jnp.bfloat16)
    second_part = jnp.dot(dense_hidden[:, half:], dense_down[half:], preferred_element_type=jnp.float32).astype(jnp.bfloat16)
    first_part, second_part = lax.optimization_barrier((first_part, second_part))
    dense_sum = first_part.astype(jnp.float32) + second_part.astype(jnp.float32)
    return (combined + jax.nn.sigmoid(branch_gate)[None, :] * dense_sum).astype(jnp.bfloat16)
```

```python
import jax
import jax.numpy as jnp
from jax import lax
from jax.sharding import PartitionSpec as P

BF16 = jnp.bfloat16
F32 = jnp.float32
ROWS = "permute"
PARTS = "native"
DENSE = "mixed"
BACK = "native"
DOWN = "permute"


def exchange(blocks, axis, mode):
    count = len(blocks)
    if mode == "permute":
        return [blocks[0]] + [
            lax.ppermute(blocks[k], axis, [(i, (i + k) % count) for i in range(count)])
            for k in range(1, count)
        ]
    me = lax.axis_index(axis)
    stacked = jnp.stack(blocks)
    doubled = jnp.concatenate([stacked, stacked])
    placed = lax.dynamic_slice_in_dim(doubled, (count - me) % count, count, 0)
    arrived = lax.all_to_all(placed, axis, split_axis=0, concat_axis=0, tiled=True)
    return rolled_from(arrived, me)


def rolled_from(arrived, me):
    count = arrived.shape[0]
    return [lax.dynamic_index_in_dim(arrived, (me - k) % count, 0, keepdims=False) for k in range(count)]


def to_all(block, axis, mode):
    count = lax.axis_size(axis)
    return lax.all_to_all(
        jnp.broadcast_to(block[None], (count,) + block.shape), axis, split_axis=0, concat_axis=0, tiled=True
    )


def in_order(blocks, axis):
    count = len(blocks)
    me = lax.axis_index(axis)
    flipped = jnp.stack(blocks[::-1])
    doubled = jnp.concatenate([flipped, flipped])
    return lax.dynamic_slice_in_dim(doubled, (count - 1 - me) % count, count, 0)


def tp_sum(value):
    half = value.shape[-1] // 2
    first = lax.axis_index("tp") == 0
    low, high = value[..., :half], value[..., half:]
    kept = jnp.where(first, low, high)
    given = lax.ppermute(jnp.where(first, high, low), "tp", [(0, 1), (1, 0)])
    return kept.astype(F32) + given.astype(F32)


def local(
    tokens,
    chosen,
    route_weight,
    expert_gate,
    expert_up,
    expert_down,
    dense_gate,
    dense_up,
    dense_down,
    branch_gate,
):
    ep = lax.axis_size("ep")
    me = lax.axis_index("ep")
    experts, _, slots = chosen.shape
    members = ep // experts
    tok_local, width = tokens.shape
    picked = chosen[:, 0, :]
    hot = picked[:, :, None] == lax.broadcasted_iota(jnp.int32, (experts, slots, tok_local), 2)
    token_rows = jnp.dot(
        hot.reshape(experts * slots, tok_local).astype(BF16), tokens, preferred_element_type=F32
    ).astype(BF16).reshape(experts, slots, width)

    row_mode = ROWS if experts == 1 else "native"
    if row_mode == "permute":
        blocks = [token_rows[0]] * ep
        received = jnp.stack(exchange(blocks, "ep", "permute"))
    elif row_mode == "gather" and experts == 1:
        received = lax.all_gather(token_rows[0], "ep", axis=0)
    else:
        received = lax.all_to_all(
            jnp.repeat(token_rows, members, axis=0), "ep", split_axis=0, concat_axis=0, tiled=True
        )
    flat_rows = received.reshape(ep * slots, width)

    cut = width // ep
    half_hidden = dense_gate.shape[1]
    if DENSE == "weights":
        terms = []
        weights = jnp.concatenate([dense_gate, dense_up], axis=1)
        arrived = exchange([weights] * ep, "ep", "permute")
        both = jnp.zeros((tok_local, 2 * half_hidden), F32)
        for k in range(ep):
            part = lax.dynamic_slice_in_dim(tokens, ((me - k) % ep) * cut, cut, 1)
            both = both + jnp.dot(part, arrived[k], preferred_element_type=F32)
    else:
        pieces = jnp.transpose(tokens.reshape(tok_local, ep, cut), (1, 0, 2))
        if PARTS == "permute":
            blocks = [lax.dynamic_index_in_dim(pieces, (me + k) % ep, 0, keepdims=False) for k in range(ep)]
            mine = jnp.stack(exchange(blocks, "ep", "permute"))
        else:
            mine = lax.all_to_all(pieces, "ep", split_axis=0, concat_axis=0, tiled=True)
        mine = mine.reshape(ep * tok_local, cut)
        partial = jnp.concatenate(
            [
                jnp.dot(mine, dense_gate, preferred_element_type=F32).astype(BF16),
                jnp.dot(mine, dense_up, preferred_element_type=F32).astype(BF16),
            ],
            axis=1,
        ).reshape(ep, tok_local, 2 * half_hidden)
        if PARTS == "permute":
            sent = exchange([partial[(ep - j) % ep] for j in range(ep)], "ep", "permute")
            both = sum(value.astype(F32) for value in sent)
        else:
            both = lax.all_to_all(partial, "ep", split_axis=0, concat_axis=0, tiled=True).astype(F32).sum(axis=0)
    dense_hidden = (jax.nn.silu(both[:, :half_hidden]) * both[:, half_hidden:]).astype(BF16)

    if DENSE == "moves":
        everyone = to_all(dense_hidden, "ep", "native").reshape(ep * tok_local, half_hidden)
        parts = jnp.dot(everyone, dense_down, preferred_element_type=F32).astype(BF16)
        parts = lax.all_to_all(
            parts.reshape(ep, tok_local, cut), "ep", split_axis=0, concat_axis=0, tiled=True
        )
    elif DOWN == "permute":
        arrived = exchange([dense_down] * ep, "ep", "permute")
        parts = in_order(
            [jnp.dot(dense_hidden, shard, preferred_element_type=F32).astype(BF16) for shard in arrived], "ep"
        )
    else:
        shards = to_all(dense_down, "ep", "native")
        parts = jnp.stack(
            [jnp.dot(dense_hidden, shards[k], preferred_element_type=F32).astype(BF16) for k in range(ep)]
        )
    dense_terms = jnp.transpose(parts, (1, 0, 2)).reshape(tok_local, width)
    dense_sum = tp_sum(dense_terms)

    gate_act = jnp.dot(flat_rows, expert_gate, preferred_element_type=F32)
    up_act = jnp.dot(flat_rows, expert_up, preferred_element_type=F32)
    hidden = (jax.nn.silu(gate_act) * up_act).astype(BF16)
    block_sum = jnp.dot(hidden, expert_down, preferred_element_type=F32).astype(BF16)
    member_sum = tp_sum(block_sum).astype(BF16).reshape(ep, slots, width // 2)
    if row_mode == "permute":
        sent = exchange([member_sum[(ep - j) % ep] for j in range(ep)], "ep", "permute")
        summed = sum(value.astype(F32) for value in sent)[None]
    else:
        order = member_sum
        returned = lax.all_to_all(order, "ep", split_axis=0, concat_axis=0, tiled=True)
        summed = returned.astype(F32).reshape(experts, members, slots, width // 2).sum(axis=1)
    table = jnp.where(hot, route_weight[:, 0, :, None], 0.0)
    combined = jnp.einsum("ekt,ekf->tf", table, summed, precision=lax.Precision.HIGHEST)
    return (combined + jax.nn.sigmoid(branch_gate)[None, :] * dense_sum).astype(BF16)


def solution(mesh):
    return jax.shard_map(
        local,
        mesh=mesh,
        in_specs=(
            P(("grp", "ep"), None),
            P(None, ("grp", "ep"), None),
            P(None, ("grp", "ep"), None),
            P(None, ("ep", "tp")),
            P(None, ("ep", "tp")),
            P(("ep", "tp"), None),
            P("ep", "tp"),
            P("ep", "tp"),
            P("tp", "ep"),
            P("tp"),
        ),
        out_specs=P(("grp", "ep"), "tp"),
        check_vma=False,
    )
```

```python
import jax
import jax.numpy as jnp
from jax import lax
from jax.sharding import PartitionSpec as P

BF16 = jnp.bfloat16
F32 = jnp.float32
DOWN = "double"
FAR = True
MERGE2 = False


def swap(blocks):
    return lax.all_to_all(blocks, "ep", split_axis=0, concat_axis=0, tiled=True)


def bits_of(count):
    return [1 << at for at in reversed(range(count.bit_length() - 1))]


def collect(block, order):
    count = lax.axis_size("ep")
    held = block
    for depth, step in enumerate(order):
        theirs = lax.ppermute(held, "ep", [(i, i ^ step) for i in range(count)])
        held = jnp.stack([held, theirs], axis=depth)
    return held


def straighten(held, order):
    me = lax.axis_index("ep")
    for depth, step in enumerate(order):
        held = jnp.where(me & step != 0, jnp.flip(held, depth), held)
    wanted = sorted(range(len(order)), key=lambda depth: -order[depth])
    held = jnp.transpose(held, tuple(wanted) + tuple(range(len(order), held.ndim)))
    return held.reshape((-1,) + held.shape[len(order) :])


def tp_sum(value):
    half = value.shape[-1] // 2
    first = lax.axis_index("tp") == 0
    low, high = value[..., :half], value[..., half:]
    kept = jnp.where(first, low, high)
    given = lax.ppermute(jnp.where(first, high, low), "tp", [(0, 1), (1, 0)])
    return kept.astype(F32) + given.astype(F32)


def local(
    tokens,
    chosen,
    route_weight,
    expert_gate,
    expert_up,
    expert_down,
    dense_gate,
    dense_up,
    dense_down,
    branch_gate,
):
    ep = lax.axis_size("ep")
    experts, _, slots = chosen.shape
    members = ep // experts
    tok_local, width = tokens.shape
    cut = width // ep
    hidden_local = dense_gate.shape[1]
    picked = chosen[:, 0, :]
    hot = picked[:, :, None] == lax.broadcasted_iota(jnp.int32, (experts, slots, tok_local), 2)
    token_rows = jnp.dot(
        hot.reshape(experts * slots, tok_local).astype(BF16), tokens, preferred_element_type=F32
    ).astype(BF16)

    order = bits_of(ep)
    if DOWN == "double":
        down_order = order if FAR else order[::-1]
        held = collect(dense_down, down_order)
    if experts == 1:
        flat_rows = straighten(collect(token_rows, order), order).reshape(ep * slots, width)
    else:
        rows_out = jnp.repeat(token_rows.reshape(experts, slots * ep, cut), members, axis=0)
        flat_rows = swap(rows_out).reshape(ep * slots, width)
    pieces_out = jnp.transpose(tokens.reshape(tok_local, ep, cut), (1, 0, 2))
    pieces = swap(pieces_out).reshape(ep * tok_local, cut)
    if DOWN == "permute":
        me = lax.axis_index("ep")
        shards = [dense_down] + [
            lax.ppermute(dense_down, "ep", [(i, (i + k) % ep) for i in range(ep)]) for k in range(1, ep)
        ]

    gate_part = jnp.dot(pieces, dense_gate, preferred_element_type=F32).astype(BF16)
    up_part = jnp.dot(pieces, dense_up, preferred_element_type=F32).astype(BF16)
    partial = jnp.concatenate([gate_part, up_part], axis=1).reshape(ep, tok_local, 2 * hidden_local)

    gate_act = jnp.dot(flat_rows, expert_gate, preferred_element_type=F32)
    up_act = jnp.dot(flat_rows, expert_up, preferred_element_type=F32)
    hidden = (jax.nn.silu(gate_act) * up_act).astype(BF16)
    block_sum = jnp.dot(hidden, expert_down, preferred_element_type=F32).astype(BF16)
    member_sum = tp_sum(block_sum).astype(BF16)

    if MERGE2:
        back_lines = slots * (width // 2) // (2 * hidden_local)
        returned = swap(
            jnp.concatenate([partial, member_sum.reshape(ep, back_lines, 2 * hidden_local)], axis=1)
        )
        both = returned[:, :tok_local].astype(F32).sum(axis=0)
        back = returned[:, tok_local:].astype(F32)
        summed = back.reshape(experts, members, back_lines, 2 * hidden_local).sum(axis=1)
        summed = summed.reshape(experts, slots, width // 2)
    else:
        both = swap(partial).astype(F32).sum(axis=0)
        back_lines = slots * (width // 2) // (2 * hidden_local)
        back = swap(member_sum.reshape(ep, back_lines, 2 * hidden_local)).astype(F32)
        summed = back.reshape(experts, members, back_lines, 2 * hidden_local).sum(axis=1)
        summed = summed.reshape(experts, slots, width // 2)
    dense_hidden = (jax.nn.silu(both[:, :hidden_local]) * both[:, hidden_local:]).astype(BF16)

    if DOWN == "moves":
        everyone = straighten(collect(dense_hidden, order), order)
        parts = jnp.dot(
            everyone.reshape(ep * tok_local, hidden_local), dense_down, preferred_element_type=F32
        ).astype(BF16)
        parts = swap(parts.reshape(ep, tok_local, cut))
    elif DOWN == "permute":
        found = [jnp.dot(dense_hidden, shard, preferred_element_type=F32).astype(BF16) for shard in shards]
        flipped = jnp.stack(found[::-1])
        doubled = jnp.concatenate([flipped, flipped])
        parts = lax.dynamic_slice_in_dim(doubled, (ep - 1 - me) % ep, ep, 0)
    else:
        shards = held.reshape((ep,) + dense_down.shape)
        parts = jnp.stack(
            [jnp.dot(dense_hidden, shards[k], preferred_element_type=F32).astype(BF16) for k in range(ep)]
        )
        parts = straighten(parts.reshape(held.shape[: len(order)] + parts.shape[1:]), down_order)
    dense_sum = tp_sum(jnp.transpose(parts, (1, 0, 2)).reshape(tok_local, width))
    table = jnp.where(hot, route_weight[:, 0, :, None], 0.0)
    combined = jnp.einsum("ekt,ekf->tf", table, summed, precision=lax.Precision.HIGHEST)
    return (combined + jax.nn.sigmoid(branch_gate)[None, :] * dense_sum).astype(BF16)


def solution(mesh):
    return jax.shard_map(
        local,
        mesh=mesh,
        in_specs=(
            P(("grp", "ep"), None),
            P(None, ("grp", "ep"), None),
            P(None, ("grp", "ep"), None),
            P(None, ("ep", "tp")),
            P(None, ("ep", "tp")),
            P(("ep", "tp"), None),
            P("ep", "tp"),
            P("ep", "tp"),
            P("tp", "ep"),
            P("tp"),
        ),
        out_specs=P(("grp", "ep"), "tp"),
        check_vma=False,
    )
```

```python
import jax
import jax.numpy as jnp
from jax import lax
from jax.sharding import PartitionSpec as P

BF16 = jnp.bfloat16
F32 = jnp.float32


def swap(blocks):
    return lax.all_to_all(blocks, "ep", split_axis=0, concat_axis=0, tiled=True)


def bits_of(count):
    return [1 << at for at in reversed(range(count.bit_length() - 1))]


def collect(block, order):
    count = lax.axis_size("ep")
    held = block
    for depth, step in enumerate(order):
        theirs = lax.ppermute(held, "ep", [(i, i ^ step) for i in range(count)])
        held = jnp.stack([held, theirs], axis=depth)
    return held


def straighten(held, order):
    me = lax.axis_index("ep")
    for depth, step in enumerate(order):
        held = jnp.where(me & step != 0, jnp.flip(held, depth), held)
    wanted = sorted(range(len(order)), key=lambda depth: -order[depth])
    held = jnp.transpose(held, tuple(wanted) + tuple(range(len(order), held.ndim)))
    return held.reshape((-1,) + held.shape[len(order) :])


def tp_sum(value):
    half = value.shape[-1] // 2
    first = lax.axis_index("tp") == 0
    low, high = value[..., :half], value[..., half:]
    kept = jnp.where(first, low, high)
    given = lax.ppermute(jnp.where(first, high, low), "tp", [(0, 1), (1, 0)])
    return kept.astype(F32) + given.astype(F32)


def layer(
    tokens,
    chosen,
    route_weight,
    expert_gate,
    expert_up,
    expert_down,
    dense_gate,
    dense_up,
    dense_down,
    branch_gate,
):
    ep = lax.axis_size("ep")
    experts, _, slots = chosen.shape
    members = ep // experts
    tok_local, width = tokens.shape
    cut = width // ep
    hidden_local = dense_gate.shape[1]
    picked = chosen[:, 0, :]
    hot = picked[:, :, None] == lax.broadcasted_iota(jnp.int32, (experts, slots, tok_local), 2)
    token_rows = jnp.dot(
        hot.reshape(experts * slots, tok_local).astype(BF16), tokens, preferred_element_type=F32
    ).astype(BF16)

    order = bits_of(ep)
    down_order = order
    held = collect(dense_down, down_order)
    if experts == 1:
        flat_rows = straighten(collect(token_rows, order), order).reshape(ep * slots, width)
    else:
        rows_out = jnp.repeat(token_rows.reshape(experts, slots * ep, cut), members, axis=0)
        flat_rows = swap(rows_out).reshape(ep * slots, width)
    pieces_out = jnp.transpose(tokens.reshape(tok_local, ep, cut), (1, 0, 2))
    pieces = swap(pieces_out).reshape(ep * tok_local, cut)

    gate_part = jnp.dot(pieces, dense_gate, preferred_element_type=F32).astype(BF16)
    up_part = jnp.dot(pieces, dense_up, preferred_element_type=F32).astype(BF16)
    partial = jnp.concatenate([gate_part, up_part], axis=1).reshape(ep, tok_local, 2 * hidden_local)

    gate_act = jnp.dot(flat_rows, expert_gate, preferred_element_type=F32)
    up_act = jnp.dot(flat_rows, expert_up, preferred_element_type=F32)
    hidden = (jax.nn.silu(gate_act) * up_act).astype(BF16)
    block_sum = jnp.dot(hidden, expert_down, preferred_element_type=F32).astype(BF16)
    member_sum = tp_sum(block_sum).astype(BF16)

    both = swap(partial).astype(F32).sum(axis=0)
    back_lines = slots * (width // 2) // (2 * hidden_local)
    back = swap(member_sum.reshape(ep, back_lines, 2 * hidden_local)).astype(F32)
    summed = back.reshape(experts, members, back_lines, 2 * hidden_local).sum(axis=1)
    summed = summed.reshape(experts, slots, width // 2)
    dense_hidden = (jax.nn.silu(both[:, :hidden_local]) * both[:, hidden_local:]).astype(BF16)

    shards = held.reshape((ep,) + dense_down.shape)
    parts = jnp.stack(
        [jnp.dot(dense_hidden, shards[k], preferred_element_type=F32).astype(BF16) for k in range(ep)]
    )
    parts = straighten(parts.reshape(held.shape[: len(order)] + parts.shape[1:]), down_order)
    dense_sum = tp_sum(jnp.transpose(parts, (1, 0, 2)).reshape(tok_local, width))
    table = jnp.where(hot, route_weight[:, 0, :, None], 0.0)
    combined = jnp.einsum("ekt,ekf->tf", table, summed, precision=lax.Precision.HIGHEST)
    return (combined + jax.nn.sigmoid(branch_gate)[None, :] * dense_sum).astype(BF16)


def solution(mesh):
    return jax.shard_map(
        layer,
        mesh=mesh,
        in_specs=(
            P(("grp", "ep"), None),
            P(None, ("grp", "ep"), None),
            P(None, ("grp", "ep"), None),
            P(None, ("ep", "tp")),
            P(None, ("ep", "tp")),
            P(("ep", "tp"), None),
            P("ep", "tp"),
            P("ep", "tp"),
            P("tp", "ep"),
            P("tp"),
        ),
        out_specs=P(("grp", "ep"), "tp"),
        check_vma=False,
    )
```
